128 devices in a mesh: ep: 128 (over z, y, x, core).
Axes of the slice: x: 4, y: 4, z: 4, core: 2. Of those that a mesh axis runs over, the one named last changes fastest.
Arguments:
- tokens: bfloat16 [32768, 2048], P('ep'), may hold values from -6 to 6
- norm_gain: float32 [2048], replicated, may hold values from 0.1 to 1.9
- expert_ids: int32 [32768, 2], P('ep'), may hold values from 0 to 127, as said below
- gates: float32 [32768, 2], P('ep'), may hold values from 0.1 to 1
- w_gate: bfloat16 [128, 2048, 1024], P('ep'), may hold values from -0.125 to 0.125
- w_up: bfloat16 [128, 2048, 1024], P('ep'), may hold values from -0.125 to 0.125
- w_down: bfloat16 [128, 1024, 2048], P('ep'), may hold values from -0.1875 to 0.1875
Outputs:
- combined: bfloat16 [32768, 2048], P('ep')
The draws below stay inside these ranges and needn't reach their ends.
Inputs may be any that keep to these rules, and one draw needn't show every extreme that they name: `expert_ids`: each row names two different experts of one group, a group being 4 consecutive expert numbers. Among the rows of one device no expert is named more than 8 times, and some expert is named exactly 8 times; some expert is named exactly 8 times by the rows of every device.
All inputs are finite; a program needn't handle non-finite values.
Results may differ from the reference program's by a relative error of at most 0.0085.
Values may be sent and summed in bfloat16 or wider, within the bound.
A program may use at most 128 MiB of HBM per device.

```python
import jax
import jax.numpy as jnp
from jax import lax

D = 2048
FF = 1024
GROUP_EXPERTS = 4
TOK_DEV = 256
EXPERTS = 128
CAP = 8
TOKENS = 32768
N_EP = 128


def draw_expert_ids(key, part):
    groups = EXPERTS // GROUP_EXPERTS
    pool_size = groups * 2 * CAP
    popularity = jax.random.randint(jax.random.fold_in(key, 11), (groups,), 0, 4)
    common = jax.random.randint(jax.random.fold_in(key, 13), (), 0, groups)
    slot_group = jnp.arange(pool_size, dtype=jnp.int32) // (2 * CAP)
    slot_position = jnp.arange(pool_size, dtype=jnp.int32) % (2 * CAP)

    def one_block(block_index):
        subkeys = jax.random.split(jax.random.fold_in(jax.random.fold_in(key, 17), block_index), 5)
        chosen_group = jax.random.randint(subkeys[0], (), 0, groups)
        jitter = jax.random.randint(subkeys[1], (pool_size,), 0, 4096)
        priority = popularity[slot_group] * 2048 + jitter
        priority = jnp.where(slot_group == chosen_group, 16384 + jitter, priority)
        priority = jnp.where(slot_group == common, 32768 + jitter, priority)
        priority = priority * pool_size + jnp.arange(pool_size, dtype=jnp.int32)
        _, picked = lax.top_k(priority, TOK_DEV)
        picked = picked[jax.random.permutation(subkeys[2], TOK_DEV)]
        group_of = slot_group[picked]
        position = slot_position[picked]
        ranks = jax.random.randint(subkeys[3], (groups, GROUP_EXPERTS), 0, 1 << 20) * GROUP_EXPERTS
        orders = jnp.argsort(ranks + jnp.arange(GROUP_EXPERTS, dtype=jnp.int32)[None, :], axis=1)
        rotation = jax.random.randint(subkeys[4], (groups,), 0, 3)
        quarter = position % 4
        offset = 1 + (position // 4 + rotation[group_of]) % 3
        first_local = orders[group_of, quarter]
        second = orders[group_of, (quarter + offset) % 4]
        return jnp.stack([group_of * GROUP_EXPERTS + first_local, group_of * GROUP_EXPERTS + second], axis=1).astype(jnp.int32)
    drawn = jax.vmap(one_block)(jnp.arange(TOKENS // TOK_DEV, dtype=jnp.int32))
    return drawn.reshape(TOKENS, 2).astype(jnp.int32)


def levels(own_key, shape, shards, low, top_value):
    def one(dim, shards_of):
        steps = jax.random.uniform(jax.random.fold_in(jax.random.fold_in(own_key, 6), dim), (shards_of,), jnp.float32, low / len(shards), top_value / len(shards))
        return jnp.repeat(jnp.exp(steps), shape[dim] // shards_of).reshape((-1,) + (1,) * (len(shape) - dim - 1))

    level = one(*shards[0])
    for cut in shards[1:]:
        level = level * one(*cut)
    return level


def scatter_about(rng, dims, deviation, reach, pieces=(), kind=jnp.bfloat16):
    values = jax.random.normal(rng, dims, jnp.float32) * deviation
    if len(pieces) > 0:
        values = levels(rng, dims, pieces, -0.22, 0.18) * values
    return jnp.clip(values, min=-reach, max=reach).astype(kind)


def setup_inputs(seed: int = 0) -> dict:
    splits = jax.random.split(jax.random.key(seed), 8)
    return {
        "tokens": scatter_about(splits[0], (TOKENS, D), 1.0, 6.0, ((0, 128),)),
        "norm_gain": jnp.clip(1.0 + 0.18 * jax.random.normal(splits[1], (D,), jnp.float32), 0.1, 1.9),
        "expert_ids": draw_expert_ids(jax.random.fold_in(splits[7], 71), 0),
        "gates": jnp.clip(0.1 + 0.9 * jax.random.uniform(splits[3], (TOKENS, 2), jnp.float32) ** levels(splits[3], (TOKENS, 2), ((0, 128),), -0.2, 0.2), 0.1, 1.0),
        "w_gate": scatter_about(splits[4], (EXPERTS, D, FF), D ** -0.5, 0.125, ((0, 128),)),
        "w_up": scatter_about(splits[5], (EXPERTS, D, FF), D ** -0.5, 0.125, ((0, 128),)),
        "w_down": scatter_about(splits[6], (EXPERTS, FF, D), FF ** -0.5, 0.1875, ((0, 128),)),
    }


EPS = 1e-06

def normalize(tokens, norm_gain):
    floats = tokens.astype(jnp.float32)
    inverse_rms = lax.rsqrt(lax.optimization_barrier(jnp.mean(floats * floats, axis=-1, keepdims=True)) + EPS)
    return (floats * inverse_rms * norm_gain.astype(jnp.float32)).astype(jnp.bfloat16)

def expert_rows(block_rows, gate_weight, up_weight, down_weight):
    gate_part = jnp.dot(block_rows, gate_weight, preferred_element_type=jnp.float32)
    up_part = jnp.dot(block_rows, up_weight, preferred_element_type=jnp.float32)
    hidden = (jax.nn.silu(gate_part) * up_part).astype(jnp.bfloat16)
    return jnp.dot(hidden, down_weight, preferred_element_type=jnp.float32).astype(jnp.bfloat16)

def reference(tokens, norm_gain, expert_ids, gates, w_gate, w_up, w_down):
    normed = normalize(tokens, norm_gain)
    blocks = N_EP
    grouped_ids = expert_ids.astype(jnp.int32).reshape(blocks, 2 * TOK_DEV)
    one_hot = (grouped_ids[:, :, None] == jnp.arange(EXPERTS, dtype=jnp.int32)[None, None, :]).astype(jnp.int32)
    earlier = jnp.cumsum(one_hot, axis=1) - one_hot
    slot_index = lax.optimization_barrier(jnp.sum(earlier * one_hot, axis=2)).astype(jnp.int32)
    block_index = jnp.arange(blocks, dtype=jnp.int32)[:, None]
    buffer_row = ((grouped_ids * blocks + block_index) * CAP + slot_index).reshape(-1).astype(jnp.int32)
    token_row = (jnp.arange(2 * TOKENS, dtype=jnp.int32) // 2).astype(jnp.int32)
    source_row = jnp.full((EXPERTS * blocks * CAP,), TOKENS, jnp.int32).at[buffer_row].set(token_row)
    source_row = source_row.reshape(EXPERTS, blocks * CAP)
    weight_row = jnp.zeros((EXPERTS * blocks * CAP,), jnp.float32).at[buffer_row].set(gates.reshape(-1).astype(jnp.float32))
    weight_row = weight_row.reshape(EXPERTS, blocks * CAP)
    padded = jnp.concatenate([normed, jnp.zeros((1, D), jnp.bfloat16)], axis=0)

    def add_expert(accumulated, inputs):
        rows_index, row_weight, gate_weight, up_weight, down_weight = inputs
        block_rows = jnp.take(padded, rows_index, axis=0)
        produced = expert_rows(block_rows, gate_weight, up_weight, down_weight)
        update = row_weight[:, None] * produced.astype(jnp.float32)
        return (accumulated.at[rows_index].add(update), None)
    initial = jnp.zeros((TOKENS + 1, D), jnp.float32)
    accumulated, _ = lax.scan(add_expert, initial, (source_row, weight_row, w_gate, w_up, w_down))
    return accumulated[:TOKENS].astype(jnp.bfloat16)
```

```python
import jax
import jax.numpy as jnp
from jax import lax
from jax.experimental import pallas as pl
from jax.experimental.pallas import tpu as pltpu
from jax.sharding import PartitionSpec as P

EPS = 1e-06
F32 = jnp.float32
BF16 = jnp.bfloat16


def iota(shape, dim):
    return lax.broadcasted_iota(jnp.int32, shape, dim)


def ones_where(mask):
    return jnp.where(mask, 1.0, 0.0).astype(BF16)


def dot(a, b):
    return jnp.dot(a, b, preferred_element_type=F32)


def pack_kernel(tokens_ref, gain_ref, ids_ref, out_ref, normed_ref, pick_ref):
    rows, width = tokens_ref.shape
    slots = out_ref.shape[0]
    experts = slots // 8
    floats = tokens_ref[...].astype(F32)
    mean = jnp.sum(floats * floats, axis=1, keepdims=True) * (1.0 / width)
    normed_ref[...] = (floats * lax.rsqrt(mean + EPS) * gain_ref[...]).astype(BF16)
    expert = iota((experts, rows), 0)
    named = (expert == ids_ref[0:1, :]) | (expert == ids_ref[1:2, :])
    before = ones_where(iota((rows, rows), 0) < iota((rows, rows), 1))
    rank = dot(ones_where(named), before)
    rank = jnp.where(named, rank, -1.0).astype(BF16)
    spread = ones_where(iota((slots, experts), 0) // 8 == iota((slots, experts), 1))
    slot = (iota((slots, rows), 0) % 8).astype(F32)
    pick_ref[...] = ones_where(dot(spread, rank) == slot)
    for start in range(0, width, 512):
        columns = pl.ds(start, 512)
        out_ref[:, columns] = dot(pick_ref[...], normed_ref[:, columns]).astype(BF16)


def combine_kernel(results_ref, ids_ref, gates_ref, out_ref, first_ref, second_ref):
    slots, width = results_ref.shape
    rows = out_ref.shape[0]
    experts = slots // 8
    expert = iota((rows, experts), 1)
    first, second = ids_ref[:, 0:1], ids_ref[:, 1:2]
    named = (expert == first) | (expert == second)
    before = ones_where(iota((rows, rows), 1) < iota((rows, rows), 0))
    rank = dot(before, ones_where(named))
    rank = jnp.where(named, rank, -1.0).astype(BF16)
    spread = ones_where(iota((experts, slots), 1) // 8 == iota((experts, slots), 0))
    column = iota((rows, slots), 1)
    held = dot(rank, spread) == (column % 8).astype(F32)
    first_ref[...] = ones_where(held & (column // 8 == first))
    second_ref[...] = ones_where(held & (column // 8 == second))
    for start in range(0, width, 512):
        columns = pl.ds(start, 512)
        picked = results_ref[:, columns]
        total = dot(first_ref[...], picked) * gates_ref[:, 0:1] + dot(second_ref[...], picked) * gates_ref[:, 1:2]
        out_ref[:, columns] = total.astype(BF16)


def whole():
    return pl.BlockSpec(memory_space=pltpu.VMEM)


def shards(tokens, norm_gain, expert_ids, gates, w_gate, w_up, w_down):
    rows, width = tokens.shape
    experts = lax.axis_size("ep")
    slots = experts * 8
    outgoing = pl.pallas_call(
        pack_kernel,
        out_shape=jax.ShapeDtypeStruct((slots, width), BF16),
        in_specs=[whole()] * 3,
        out_specs=whole(),
        scratch_shapes=[pltpu.VMEM((rows, width), BF16), pltpu.VMEM((slots, rows), BF16)],
        compiler_params=pltpu.CompilerParams(vmem_limit_bytes=40 << 20),
        name="pack",
    )(tokens, norm_gain.reshape(1, width), expert_ids.T)
    arrived = lax.all_to_all(outgoing.reshape(experts, 8, width), "ep", split_axis=0, concat_axis=0, tiled=True)
    block_rows = arrived.reshape(slots, width)
    gate_part = dot(block_rows, w_gate[0])
    up_part = dot(block_rows, w_up[0])
    hidden = (jax.nn.silu(gate_part) * up_part).astype(BF16)
    produced = dot(hidden, w_down[0]).astype(BF16)
    returned = lax.all_to_all(produced.reshape(experts, 8, width), "ep", split_axis=0, concat_axis=0, tiled=True)
    return pl.pallas_call(
        combine_kernel,
        out_shape=jax.ShapeDtypeStruct((rows, width), BF16),
        in_specs=[whole()] * 3,
        out_specs=whole(),
        scratch_shapes=[pltpu.VMEM((rows, slots), BF16)] * 2,
        compiler_params=pltpu.CompilerParams(vmem_limit_bytes=40 << 20),
        name="combine",
    )(returned.reshape(slots, width), expert_ids, gates)


def solution(mesh):
    return jax.shard_map(
        shards,
        mesh=mesh,
        in_specs=(
            P("ep", None),
            P(),
            P("ep", None),
            P("ep", None),
            P("ep", None, None),
            P("ep", None, None),
            P("ep", None, None),
        ),
        out_specs=P("ep", None),
        check_vma=False,
    )
```

```python
import jax
import jax.numpy as jnp
from jax import lax
from jax.experimental import pallas as pl
from jax.experimental.pallas import tpu as pltpu
from jax.sharding import PartitionSpec as P

EPS = 1e-06
F32 = jnp.float32
BF16 = jnp.bfloat16
MESH = pl.DeviceIdType.MESH
SLOTS = 8
GROUP_SLOTS = 16
BATCHES = 4
RANKS = 8


def iota(shape, dim):
    return lax.broadcasted_iota(jnp.int32, shape, dim)


def ones_where(mask):
    return jnp.where(mask, 1.0, 0.0).astype(BF16)


def dot(a, b):
    return jnp.dot(a, b, preferred_element_type=F32)


def peer(me, batch, core, rank):
    dy = rank & 3
    x = ((me >> 1) & 3) ^ (3 * (rank >> 2))
    y = (((me >> 3) & 3) + dy) & 3
    z = ((me >> 5) + batch - dy) & 3
    return (z << 5) | (y << 3) | (x << 1) | ((me & 1) ^ core)


def expert_slots(ids_ref):
    rows = ids_ref.shape[1]
    first, second = ids_ref[0:1, :], ids_ref[1:2, :]
    expert = iota((128, rows), 0)
    is_first, is_second = expert == first, expert == second
    before = ones_where(iota((rows, rows), 0) < iota((rows, rows), 1))
    rank = dot(ones_where(is_first | is_second), before)
    slot_first = jnp.sum(jnp.where(is_first, rank, 0.0), axis=0, keepdims=True).astype(jnp.int32)
    slot_second = jnp.sum(jnp.where(is_second, rank, 0.0), axis=0, keepdims=True).astype(jnp.int32)
    return first, second, slot_first, slot_second


def pack(me, tokens_ref, gain_ref, ids_ref, out_ref, normed_ref):
    rows, width = tokens_ref.shape
    floats = tokens_ref[...].astype(F32)
    mean = jnp.sum(floats * floats, axis=1, keepdims=True) * (1.0 / width)
    normed_ref[...] = (floats * lax.rsqrt(mean + EPS) * gain_ref[...]).astype(BF16)
    first, second, slot_first, slot_second = expert_slots(ids_ref)
    count = BATCHES * 2 * RANKS * SLOTS
    row = iota((count, rows), 0)
    wanted = peer(me, row >> 7, (row >> 6) & 1, (row >> 3) & 7) * SLOTS + (row & 7)
    chosen = ones_where((wanted == first * SLOTS + slot_first) | (wanted == second * SLOTS + slot_second))
    for start in range(0, width, 512):
        columns = pl.ds(start, 512)
        block = dot(chosen, normed_ref[:, columns]).astype(BF16)
        out_ref[:, :, columns] = block.reshape(count // SLOTS, SLOTS, 512)


def describe(me, ids_ref, gates_ref, places_ref, meta_ref):
    rows = ids_ref.shape[1]
    first, second, slot_first, slot_second = expert_slots(ids_ref)
    group = first >> 2
    in_group = iota((32, rows), 0) == group
    before = ones_where(iota((rows, rows), 0) < iota((rows, rows), 1))
    rank = dot(ones_where(in_group), before)
    place = jnp.sum(jnp.where(in_group, rank, 0.0), axis=0, keepdims=True).astype(jnp.int32)
    side = ((me >> 1) ^ (me >> 2)) & 1
    relay = (((group & 1) ^ side) << 1) | (me & 1)
    source_first = ((first ^ relay) & 3) * 64 + slot_first
    source_second = ((second ^ relay) & 3) * 64 + slot_second
    count = BATCHES * RANKS * GROUP_SLOTS
    row = iota((count, rows), 0)
    wanted = (peer(me, row >> 7, 0, (row >> 4) & 7) >> 2) * GROUP_SLOTS + (row & 15)
    places = ones_where(wanted == group * GROUP_SLOTS + place)
    places_ref[...] = places
    values = [source_first.astype(F32), source_second.astype(F32)]
    for k in range(2):
        rest = gates_ref[k : k + 1, :]
        for _ in range(3):
            part = rest.astype(BF16).astype(F32)
            values.append(part)
            rest = rest - part
    kind = iota((128, rows), 0)
    table = jnp.zeros((128, rows), F32)
    for k, value in enumerate(values):
        table = jnp.where(kind == k, value, table)
    meta = lax.dot_general(places, table.astype(BF16), (((1,), (1,)), ((), ())), preferred_element_type=F32)
    meta_ref[...] = meta.astype(BF16).reshape(BATCHES * RANKS, GROUP_SLOTS, 128)


def layer_kernel(
    tokens_ref, gain_ref, ids_ref, gates_ref, w_gate_ref, w_up_ref, w_down_ref, out_ref,
    gate_w, up_w, down_w, near_tokens, near_ids, normed, packed, arrived, hidden, produced, gathered, places,
    meta_out, meta_in, sums, returned,
    weight_sem, raw_send, raw_recv, ids_send, ids_recv, meta_send, meta_recv, packed_send, arrived_recv,
    core_send, core_recv, cross_send, cross_recv, sums_send, returned_recv,
):
    me = lax.axis_index("ep")
    width = tokens_ref.shape[1]
    ff = hidden.shape[1]
    per_wave = BATCHES * 2 * RANKS

    def at(i):
        return peer(me, i >> 4, (i >> 3) & 1, i & 7)

    barrier = pltpu.get_barrier_semaphore()

    def greet(i, carry):
        pl.semaphore_signal(barrier, inc=1, device_id=(at(i),), device_id_type=MESH)
        return carry

    lax.fori_loop(1, per_wave, greet, 0)
    pl.semaphore_signal(barrier, inc=1, device_id=(me ^ 2,), device_id_type=MESH)
    pl.semaphore_signal(barrier, inc=1, device_id=(me ^ 3,), device_id_type=MESH)

    weights = [
        pltpu.make_async_copy(w_gate_ref.at[0], gate_w, weight_sem.at[0]),
        pltpu.make_async_copy(w_up_ref.at[0], up_w, weight_sem.at[1]),
        pltpu.make_async_copy(w_down_ref.at[0], down_w, weight_sem.at[2]),
    ]
    for copy in weights:
        copy.start()

    pl.semaphore_wait(barrier, per_wave + 1)

    raw = pltpu.make_async_remote_copy(
        tokens_ref, near_tokens, raw_send, raw_recv, device_id=(me ^ 2,), device_id_type=MESH
    )
    raw_ids = pltpu.make_async_remote_copy(
        ids_ref, near_ids, ids_send, ids_recv, device_id=(me ^ 2,), device_id_type=MESH
    )
    raw_ids.start()
    raw.start()

    def send_packed(wave):
        def send(i, carry):
            unit = wave * BATCHES + (i >> 4)
            pltpu.make_async_remote_copy(
                packed.at[wave, i], arrived.at[unit, i & 15], packed_send.at[wave], arrived_recv.at[unit],
                device_id=(at(i),), device_id_type=MESH,
            ).start()
            return carry

        lax.fori_loop(1, per_wave, send, 0)
        arrived[wave * BATCHES, 0] = packed[wave, 0]

    pack(me, tokens_ref, gain_ref, ids_ref, packed.at[0], normed)
    send_packed(0)
    describe(me, ids_ref, gates_ref, places, meta_out)

    def send_meta(i, carry):
        pltpu.make_async_remote_copy(
            meta_out.at[i], meta_in.at[i], meta_send, meta_recv,
            device_id=(peer(me, i >> 3, 0, i & 7),), device_id_type=MESH,
        ).start()
        return carry

    lax.fori_loop(1, BATCHES * RANKS, send_meta, 0)
    meta_in[0] = meta_out[0]

    for copy in weights:
        copy.wait()

    def expert(unit, carry):
        batch = unit & 3

        @pl.when(batch == 0)
        def _():
            view = arrived.at[unit, pl.ds(1, 15)]
            pltpu.make_async_copy(view, view, arrived_recv.at[unit]).wait()

        @pl.when(batch != 0)
        def _():
            view = arrived.at[unit]
            pltpu.make_async_copy(view, view, arrived_recv.at[unit]).wait()

        rows = arrived[unit].reshape(2 * RANKS * SLOTS, width)
        for start in range(0, ff, 256):
            columns = pl.ds(start, 256)
            gate_part = dot(rows, gate_w[:, columns])
            up_part = dot(rows, up_w[:, columns])
            hidden[:, columns] = (gate_part / (1.0 + jnp.exp(-gate_part)) * up_part).astype(BF16)
        for start in range(0, width, 256):
            columns = pl.ds(start, 256)
            block = dot(hidden[...], down_w[:, columns]).astype(BF16)
            produced[unit, :, :, columns] = block.reshape(2 * RANKS, SLOTS, 256)

        @pl.when(unit < BATCHES)
        def _():
            pltpu.make_async_remote_copy(
                produced.at[unit, pl.ds(RANKS, RANKS)], gathered.at[batch, 1], core_send, core_recv.at[batch],
                device_id=(me ^ 1,), device_id_type=MESH,
            ).start()
            gathered[batch, 0] = produced[unit, 0:RANKS]

        @pl.when(unit >= BATCHES)
        def _():
            for core in range(2):
                pltpu.make_async_remote_copy(
                    produced.at[unit, pl.ds(core * RANKS, RANKS)], gathered.at[batch, 2 + core],
                    cross_send.at[core], cross_recv.at[batch, core],
                    device_id=(me ^ (2 + core),), device_id_type=MESH,
                ).start()

        @pl.when(unit == 2)
        def _():
            raw_ids.wait_recv()
            raw.wait_recv()
            pack(me, near_tokens, gain_ref, near_ids, packed.at[1], normed)
            send_packed(1)

        @pl.when(unit == 6)
        def _():
            view = meta_in.at[pl.ds(1, BATCHES * RANKS - 1)]
            pltpu.make_async_copy(view, view, meta_recv).wait()

        @pl.when(unit >= 6)
        def _():
            relay(unit - 6)

        return carry

    def relay(batch):
        view = gathered.at[batch, 1]
        pltpu.make_async_copy(view, view, core_recv.at[batch]).wait()
        for core in range(2):
            view = gathered.at[batch, 2 + core]
            pltpu.make_async_copy(view, view, cross_recv.at[batch, core]).wait()
        count = RANKS * GROUP_SLOTS
        meta = meta_in[pl.ds(batch * RANKS, RANKS)].reshape(count, 128).astype(F32)
        base = (iota((count, 1), 0) // GROUP_SLOTS) * SLOTS
        column = iota((count, 4 * RANKS * SLOTS), 1)
        picks = [ones_where(column == meta[:, k : k + 1].astype(jnp.int32) + base) for k in range(2)]
        scale = [meta[:, 2 + 3 * k : 3 + 3 * k] + meta[:, 3 + 3 * k : 4 + 3 * k] + meta[:, 4 + 3 * k : 5 + 3 * k] for k in range(2)]
        for start in range(0, width, 512):
            columns = pl.ds(start, 512)
            rows = gathered[batch, :, :, :, columns].reshape(4 * RANKS * SLOTS, 512)
            total = dot(picks[0], rows) * scale[0] + dot(picks[1], rows) * scale[1]
            sums[batch, :, :, columns] = total.astype(BF16).reshape(RANKS, GROUP_SLOTS, 512)

        def send(rank, carry):
            pltpu.make_async_remote_copy(
                sums.at[batch, rank], returned.at[batch, rank], sums_send.at[batch], returned_recv.at[batch],
                device_id=(back(batch, rank),), device_id_type=MESH,
            ).start()
            return carry

        @pl.when(batch == 0)
        def _():
            returned[0, 0] = sums[0, 0]
            lax.fori_loop(1, RANKS, send, 0)

        @pl.when(batch != 0)
        def _():
            lax.fori_loop(0, RANKS, send, 0)

    def back(batch, rank):
        dy = rank & 3
        x = ((me >> 1) & 3) ^ (3 * (rank >> 2))
        y = (((me >> 3) & 3) - dy) & 3
        z = ((me >> 5) - batch + dy) & 3
        return (z << 5) | (y << 3) | (x << 1) | (me & 1)

    lax.fori_loop(0, 2 * BATCHES, expert, 0)

    def relay_step(batch, carry):
        relay(batch)
        return carry

    lax.fori_loop(2, BATCHES, relay_step, 0)

    for batch in range(BATCHES):
        view = returned.at[batch, pl.ds(1, RANKS - 1)] if batch == 0 else returned.at[batch]
        pltpu.make_async_copy(view, view, returned_recv.at[batch]).wait()
    chosen = places[...]
    for start in range(0, width, 512):
        columns = pl.ds(start, 512)
        rows = returned[:, :, :, columns].reshape(BATCHES * RANKS * GROUP_SLOTS, 512)
        block = lax.dot_general(chosen, rows, (((0,), (0,)), ((), ())), preferred_element_type=F32)
        out_ref[:, columns] = block.astype(BF16)

    raw.wait_send()
    raw_ids.wait_send()

    def drain(view, sem):
        pltpu.make_async_copy(view, view, sem).wait()

    for wave in range(2):
        drain(packed.at[wave, pl.ds(1, per_wave - 1)], packed_send.at[wave])
    drain(meta_out.at[pl.ds(1, BATCHES * RANKS - 1)], meta_send)
    drain(gathered.at[:, 1], core_send)
    for core in range(2):
        drain(gathered.at[:, 2 + core], cross_send.at[core])
    for batch in range(BATCHES):
        drain(sums.at[batch, pl.ds(1, RANKS - 1)] if batch == 0 else sums.at[batch], sums_send.at[batch])


def whole():
    return pl.BlockSpec(memory_space=pltpu.VMEM)


def shards(tokens, norm_gain, expert_ids, gates, w_gate, w_up, w_down):
    rows, width = tokens.shape
    ff = w_gate.shape[2]
    dma = pltpu.SemaphoreType.DMA
    return pl.pallas_call(
        layer_kernel,
        out_shape=jax.ShapeDtypeStruct((rows, width), BF16),
        in_specs=[whole()] * 4 + [pl.BlockSpec(memory_space=pl.ANY)] * 3,
        out_specs=whole(),
        scratch_shapes=[
            pltpu.VMEM((width, ff), BF16),
            pltpu.VMEM((width, ff), BF16),
            pltpu.VMEM((ff, width), BF16),
            pltpu.VMEM((rows, width), BF16),
            pltpu.VMEM((2, rows), jnp.int32),
            pltpu.VMEM((rows, width), BF16),
            pltpu.VMEM((2, BATCHES * 2 * RANKS, SLOTS, width), BF16),
            pltpu.VMEM((2 * BATCHES, 2 * RANKS, SLOTS, width), BF16),
            pltpu.VMEM((2 * RANKS * SLOTS, ff), BF16),
            pltpu.VMEM((2 * BATCHES, 2 * RANKS, SLOTS, width), BF16),
            pltpu.VMEM((BATCHES, 4, RANKS, SLOTS, width), BF16),
            pltpu.VMEM((BATCHES * RANKS * GROUP_SLOTS, rows), BF16),
            pltpu.VMEM((BATCHES * RANKS, GROUP_SLOTS, 128), BF16),
            pltpu.VMEM((BATCHES * RANKS, GROUP_SLOTS, 128), BF16),
            pltpu.VMEM((BATCHES, RANKS, GROUP_SLOTS, width), BF16),
            pltpu.VMEM((BATCHES, RANKS, GROUP_SLOTS, width), BF16),
            dma((3,)), dma, dma, dma, dma, dma, dma, dma((2,)), dma((2 * BATCHES,)),
            dma, dma((BATCHES,)), dma((2,)), dma((BATCHES, 2)), dma((BATCHES,)), dma((BATCHES,)),
        ],
        compiler_params=pltpu.CompilerParams(
            collective_id=0, has_side_effects=True, vmem_limit_bytes=60 << 20
        ),
        name="layer",
    )(tokens, norm_gain.reshape(1, width), expert_ids.T, gates.T, w_gate, w_up, w_down)


def solution(mesh):
    return jax.shard_map(
        shards,
        mesh=mesh,
        in_specs=(
            P("ep", None),
            P(),
            P("ep", None),
            P("ep", None),
            P("ep", None, None),
            P("ep", None, None),
            P("ep", None, None),
        ),
        out_specs=P("ep", None),
        check_vma=False,
    )
```

```python
import jax
import jax.numpy as jnp
from jax import lax
from jax.experimental import pallas as pl
from jax.experimental.pallas import tpu as pltpu
from jax.sharding import PartitionSpec as P

EPS = 1e-06
F32 = jnp.float32
BF16 = jnp.bfloat16
MESH = pl.DeviceIdType.MESH
SLOTS = 8
GROUP_SLOTS = 16
BATCHES = 4
RANKS = 8


def iota(shape, dim):
    return lax.broadcasted_iota(jnp.int32, shape, dim)


def ones_where(mask):
    return jnp.where(mask, 1.0, 0.0).astype(BF16)


def dot(a, b):
    return jnp.dot(a, b, preferred_element_type=F32)


def turns(batch):
    return batch ^ (batch >> 1)


def peer(me, batch, core, rank):
    dy = rank & 3
    x = ((me >> 1) & 3) ^ (3 * (rank >> 2))
    y = (((me >> 3) & 3) + dy) & 3
    z = ((me >> 5) + turns(batch) - dy) & 3
    return (z << 5) | (y << 3) | (x << 1) | ((me & 1) ^ core)


def expert_slots(ids_ref):
    rows = ids_ref.shape[1]
    first, second = ids_ref[0:1, :], ids_ref[1:2, :]
    expert = iota((128, rows), 0)
    is_first, is_second = expert == first, expert == second
    before = ones_where(iota((rows, rows), 0) < iota((rows, rows), 1))
    rank = dot(ones_where(is_first | is_second), before)
    slot_first = jnp.sum(jnp.where(is_first, rank, 0.0), axis=0, keepdims=True).astype(jnp.int32)
    slot_second = jnp.sum(jnp.where(is_second, rank, 0.0), axis=0, keepdims=True).astype(jnp.int32)
    return first, second, slot_first, slot_second


def normalize(tokens_ref, gain_ref, normed_ref, start, count):
    rows = pl.ds(start, count)
    floats = tokens_ref[rows, :].astype(F32)
    mean = jnp.sum(floats * floats, axis=1, keepdims=True) * (1.0 / floats.shape[1])
    normed_ref[rows, :] = (floats * lax.rsqrt(mean + EPS) * gain_ref[...]).astype(BF16)


def choose(me, ids_ref, chosen_ref):
    count, rows = chosen_ref.shape
    first, second, slot_first, slot_second = expert_slots(ids_ref)
    row = iota((count, rows), 0)
    wanted = peer(me, row >> 7, (row >> 6) & 1, (row >> 3) & 7) * SLOTS + (row & 7)
    chosen_ref[...] = ones_where((wanted == first * SLOTS + slot_first) | (wanted == second * SLOTS + slot_second))


def lay_out(chosen_ref, normed_ref, out_ref, half):
    blocks = out_ref.shape[0] // 2
    rows = pl.ds(half * blocks * SLOTS, blocks * SLOTS)
    for start in range(0, normed_ref.shape[1], 512):
        columns = pl.ds(start, 512)
        block = dot(chosen_ref[rows, :], normed_ref[:, columns]).astype(BF16)
        out_ref[pl.ds(half * blocks, blocks), :, columns] = block.reshape(blocks, SLOTS, 512)


def describe(me, ids_ref, gates_ref, places_ref, meta_ref):
    rows = ids_ref.shape[1]
    first, second, slot_first, slot_second = expert_slots(ids_ref)
    group = first >> 2
    in_group = iota((32, rows), 0) == group
    before = ones_where(iota((rows, rows), 0) < iota((rows, rows), 1))
    rank = dot(ones_where(in_group), before)
    place = jnp.sum(jnp.where(in_group, rank, 0.0), axis=0, keepdims=True).astype(jnp.int32)
    side = ((me >> 1) ^ (me >> 2)) & 1
    relay = (((group & 1) ^ side) << 1) | (me & 1)
    source_first = ((first ^ relay) & 3) * 64 + slot_first
    source_second = ((second ^ relay) & 3) * 64 + slot_second
    count = BATCHES * RANKS * GROUP_SLOTS
    row = iota((count, rows), 0)
    wanted = (peer(me, row >> 7, 0, (row >> 4) & 7) >> 2) * GROUP_SLOTS + (row & 15)
    places = ones_where(wanted == group * GROUP_SLOTS + place)
    places_ref[...] = places
    values = [source_first.astype(F32), source_second.astype(F32)]
    for k in range(2):
        rest = gates_ref[k : k + 1, :]
        for _ in range(3):
            part = rest.astype(BF16).astype(F32)
            values.append(part)
            rest = rest - part
    kind = iota((128, rows), 0)
    table = jnp.zeros((128, rows), F32)
    for k, value in enumerate(values):
        table = jnp.where(kind == k, value, table)
    meta = lax.dot_general(places, table.astype(BF16), (((1,), (1,)), ((), ())), preferred_element_type=F32)
    meta_ref[...] = meta.astype(BF16).reshape(BATCHES * RANKS, GROUP_SLOTS, 128)


def layer_kernel(
    tokens_ref, gain_hbm, ids_hbm, gates_hbm, w_gate_ref, w_up_ref, w_down_ref, out_ref,
    gate_w, up_w, down_w, gain_ref, ids_ref, gates_ref, own_tokens, near_tokens, near_ids, normed, chosen, packed,
    arrived, hidden, produced, gathered, places, meta_out, meta_in, sums, returned,
    weight_sem, load_sem, turn_sem, raw_send, raw_recv, ids_send, ids_recv, meta_send, meta_recv,
    packed_send, arrived_recv, core_send, core_recv, cross_send, cross_recv, sums_send, returned_recv,
):
    me = lax.axis_index("ep")
    core = me & 1
    rows, width = own_tokens.shape
    ff = hidden.shape[1]
    per_wave = BATCHES * 2 * RANKS

    barrier = pltpu.get_barrier_semaphore()

    def greet(device):
        pl.semaphore_signal(barrier, inc=1, device_id=(device,), device_id_type=MESH)

    def greet_plane(i, carry):
        plane = ((me + (i << 5)) & 96) | ((me + ((i >> 2) << 3)) & 24)
        for flip in (7, 6, 1):
            greet(plane | ((me & 7) ^ flip))

        @pl.when(i != 0)
        def _():
            greet(plane | (me & 7))

        return carry

    lax.fori_loop(0, 16, greet_plane, 0)
    greet(me ^ 2)
    greet(me ^ 3)

    loads = [
        pltpu.make_async_copy(ids_hbm, ids_ref, load_sem.at[0]),
        pltpu.make_async_copy(tokens_ref, own_tokens, load_sem.at[1]),
        pltpu.make_async_copy(gain_hbm, gain_ref, load_sem.at[2]),
        pltpu.make_async_copy(gates_hbm, gates_ref, load_sem.at[3]),
    ]
    weights = [
        pltpu.make_async_copy(w_gate_ref.at[0], gate_w, weight_sem.at[0]),
        pltpu.make_async_copy(w_up_ref.at[0], up_w, weight_sem.at[1]),
        pltpu.make_async_copy(w_down_ref.at[0], down_w, weight_sem.at[2]),
    ]
    for copy in loads:
        copy.start()

    chunks = [(0, 3 * rows // 8), (3 * rows // 8, 3 * rows // 8), (3 * rows // 4, rows // 8), (7 * rows // 8, rows // 8)]
    raw = [
        pltpu.make_async_remote_copy(
            tokens_ref.at[pl.ds(start, count)], near_tokens.at[pl.ds(start, count)], raw_send.at[k], raw_recv.at[k],
            device_id=(me ^ 2,), device_id_type=MESH,
        )
        for k, (start, count) in enumerate(chunks)
    ]
    raw_ids = pltpu.make_async_remote_copy(
        ids_hbm, near_ids, ids_send, ids_recv, device_id=(me ^ 2,), device_id_type=MESH
    )

    def send_packed(wave, half):
        first_unit = BATCHES * (3 * core if wave == 0 else 1 + core)
        blocks = per_wave // 2

        def send(i, carry):
            batch, rank = i >> 4, i & 7
            pltpu.make_async_remote_copy(
                packed.at[wave, i], arrived.at[first_unit + batch, rank],
                packed_send.at[wave], arrived_recv.at[first_unit + batch],
                device_id=(peer(me, batch, (i >> 3) & 1, rank),), device_id_type=MESH,
            ).start()
            return carry

        lax.fori_loop(max(1, half * blocks), (half + 1) * blocks, send, 0)
        if half == 0:
            arrived[first_unit, 0] = packed[wave, 0]

    def wait_barrier():
        with jax.named_scope("barrier"):
            pl.semaphore_wait(barrier, per_wave + 1)

    wait_barrier()
    raw_ids.start()

    @pl.when(core == 0)
    def _():
        for copy in raw:
            copy.start()

    for copy in loads:
        copy.wait()
    for copy in weights:
        copy.start()
    with jax.named_scope("pack_own"):
        choose(me, ids_ref, chosen)
        normalize(own_tokens, gain_ref, normed, 0, rows)
        for half in range(2):
            lay_out(chosen, normed, packed.at[0], half)

            @pl.when(core == 0)
            def _():
                send_packed(0, half)

    with jax.named_scope("describe"):
        describe(me, ids_ref, gates_ref, places, meta_out)

    def send_meta(i, carry):
        pltpu.make_async_remote_copy(
            meta_out.at[i], meta_in.at[i], meta_send, meta_recv,
            device_id=(peer(me, i >> 3, 0, i & 7),), device_id_type=MESH,
        ).start()
        return carry

    lax.fori_loop(1, BATCHES * RANKS, send_meta, 0)
    meta_in[0] = meta_out[0]
    with jax.named_scope("ids_wait"):
        raw_ids.wait_recv()
        choose(me, near_ids, chosen)

    @pl.when(core == 1)
    def _():
        with jax.named_scope("turn"):
            pl.semaphore_wait(turn_sem, 1)
        for copy in raw:
            copy.start()

    def near():
        for k, (start, count) in enumerate(chunks):
            with jax.named_scope("raw_wait"):
                raw[k].wait_recv()

            if k == 2:
                @pl.when(core == 0)
                def _():
                    pl.semaphore_signal(turn_sem, inc=1, device_id=(me ^ 1,), device_id_type=MESH)

            normalize(near_tokens, gain_ref, normed, start, count)
        with jax.named_scope("pack_near"):
            lay_out(chosen, normed, packed.at[1], 0)
            send_packed(1, 0)
            lay_out(chosen, normed, packed.at[1], 1)
            send_packed(1, 1)

        @pl.when(core == 1)
        def _():
            send_packed(0, 0)
            send_packed(0, 1)

    def wait_unit(unit, batch, source_core):
        alone = (batch == 0) & (source_core == core)

        @pl.when(alone)
        def _():
            view = arrived.at[unit, pl.ds(1, RANKS - 1)]
            pltpu.make_async_copy(view, view, arrived_recv.at[unit]).wait()

        @pl.when(jnp.logical_not(alone))
        def _():
            view = arrived.at[unit]
            pltpu.make_async_copy(view, view, arrived_recv.at[unit]).wait()

    def expert(unit, carry):
        @pl.when(unit == 6 * core)
        def _():
            near()

        batch, kind = unit & 3, unit >> 2
        source_core = kind >> 1
        crossing = (kind == 1) | (kind == 2)
        with jax.named_scope("unit_wait"):
            wait_unit(unit, batch, source_core)

        @pl.when(unit == 0)
        def _():
            for copy in weights:
                copy.wait()

        with jax.named_scope("unit"):
            block_rows = arrived[unit].reshape(RANKS * SLOTS, width)
            for start in range(0, ff, 256):
                columns = pl.ds(start, 256)
                gate_part = dot(block_rows, gate_w[:, columns])
                up_part = dot(block_rows, up_w[:, columns])
                hidden[:, columns] = (gate_part / (1.0 + jnp.exp(-gate_part)) * up_part).astype(BF16)
            for start in range(0, width, 256):
                columns = pl.ds(start, 256)
                block = dot(hidden[...], down_w[:, columns]).astype(BF16)
                produced[unit, :, :, columns] = block.reshape(RANKS, SLOTS, 256)

        other = source_core ^ core

        @pl.when(crossing)
        def _():
            pltpu.make_async_remote_copy(
                produced.at[unit], gathered.at[batch, 2 + other],
                cross_send.at[source_core], cross_recv.at[batch, other],
                device_id=(me ^ (2 + other),), device_id_type=MESH,
            ).start()

        @pl.when(jnp.logical_not(crossing) & (other == 1))
        def _():
            pltpu.make_async_remote_copy(
                produced.at[unit], gathered.at[batch, 1], core_send, core_recv.at[batch],
                device_id=(me ^ 1,), device_id_type=MESH,
            ).start()

        @pl.when(jnp.logical_not(crossing) & (other == 0))
        def _():
            gathered[batch, 0] = produced[unit]

        @pl.when(((core == 0) & (unit >= 8) & (unit < 12)) | (core == 1) & (unit >= 12))
        def _():
            relay(batch)

        return carry

    def relay(batch):
        with jax.named_scope("relay_wait"):
            @pl.when(batch == 0)
            def _():
                view = meta_in.at[pl.ds(1, BATCHES * RANKS - 1)]
                pltpu.make_async_copy(view, view, meta_recv).wait()

            view = gathered.at[batch, 1]
            pltpu.make_async_copy(view, view, core_recv.at[batch]).wait()
            for other in range(2):
                view = gathered.at[batch, 2 + other]
                pltpu.make_async_copy(view, view, cross_recv.at[batch, other]).wait()
        count = RANKS * GROUP_SLOTS
        meta = meta_in[pl.ds(batch * RANKS, RANKS)].reshape(count, 128).astype(F32)
        base = (iota((count, 1), 0) // GROUP_SLOTS) * SLOTS
        column = iota((count, 4 * RANKS * SLOTS), 1)
        picks = [ones_where(column == meta[:, k : k + 1].astype(jnp.int32) + base) for k in range(2)]
        scale = [meta[:, k : k + 1] + meta[:, k + 1 : k + 2] + meta[:, k + 2 : k + 3] for k in (2, 5)]
        for start in range(0, width, 512):
            columns = pl.ds(start, 512)
            rows = gathered[batch, :, :, :, columns].reshape(4 * RANKS * SLOTS, 512)
            total = dot(picks[0], rows) * scale[0] + dot(picks[1], rows) * scale[1]
            sums[batch, :, :, columns] = total.astype(BF16).reshape(RANKS, GROUP_SLOTS, 512)

        def send(rank, carry):
            pltpu.make_async_remote_copy(
                sums.at[batch, rank], returned.at[batch, rank], sums_send.at[batch], returned_recv.at[batch],
                device_id=(back(batch, rank),), device_id_type=MESH,
            ).start()
            return carry

        @pl.when(batch == 0)
        def _():
            returned[0, 0] = sums[0, 0]
            lax.fori_loop(1, RANKS, send, 0)

        @pl.when(batch != 0)
        def _():
            lax.fori_loop(0, RANKS, send, 0)

    def back(batch, rank):
        dy = rank & 3
        x = ((me >> 1) & 3) ^ (3 * (rank >> 2))
        y = (((me >> 3) & 3) - dy) & 3
        z = ((me >> 5) - turns(batch) + dy) & 3
        return (z << 5) | (y << 3) | (x << 1) | (me & 1)

    lax.fori_loop(0, 4 * BATCHES, expert, 0)

    with jax.named_scope("return_wait"):
        for batch in range(BATCHES):
            view = returned.at[batch, pl.ds(1, RANKS - 1)] if batch == 0 else returned.at[batch]
            pltpu.make_async_copy(view, view, returned_recv.at[batch]).wait()
    chosen = places[...]
    for start in range(0, width, 512):
        columns = pl.ds(start, 512)
        rows = returned[:, :, :, columns].reshape(BATCHES * RANKS * GROUP_SLOTS, 512)
        block = lax.dot_general(chosen, rows, (((0,), (0,)), ((), ())), preferred_element_type=F32)
        out_ref[:, columns] = block.astype(BF16)

    for copy in raw:
        copy.wait_send()
    raw_ids.wait_send()

    def drain(view, sem):
        pltpu.make_async_copy(view, view, sem).wait()

    for wave in range(2):
        drain(packed.at[wave, pl.ds(1, per_wave - 1)], packed_send.at[wave])
    drain(meta_out.at[pl.ds(1, BATCHES * RANKS - 1)], meta_send)
    drain(gathered.at[:, 1], core_send)
    for source_core in range(2):
        drain(gathered.at[:, 2], cross_send.at[source_core])
    for batch in range(BATCHES):
        drain(sums.at[batch, pl.ds(1, RANKS - 1)] if batch == 0 else sums.at[batch], sums_send.at[batch])


def whole():
    return pl.BlockSpec(memory_space=pltpu.VMEM)


def shards(tokens, norm_gain, expert_ids, gates, w_gate, w_up, w_down):
    rows, width = tokens.shape
    ff = w_gate.shape[2]
    dma = pltpu.SemaphoreType.DMA
    return pl.pallas_call(
        layer_kernel,
        out_shape=jax.ShapeDtypeStruct((rows, width), BF16),
        in_specs=[pl.BlockSpec(memory_space=pltpu.HBM)] * 7,
        out_specs=whole(),
        scratch_shapes=[
            pltpu.VMEM((width, ff), BF16),
            pltpu.VMEM((width, ff), BF16),
            pltpu.VMEM((ff, width), BF16),
            pltpu.VMEM((1, width), F32),
            pltpu.VMEM((2, rows), jnp.int32),
            pltpu.VMEM((2, rows), F32),
            pltpu.VMEM((rows, width), BF16),
            pltpu.VMEM((rows, width), BF16),
            pltpu.VMEM((2, rows), jnp.int32),
            pltpu.VMEM((rows, width), BF16),
            pltpu.VMEM((BATCHES * 2 * RANKS * SLOTS, rows), BF16),
            pltpu.VMEM((2, BATCHES * 2 * RANKS, SLOTS, width), BF16),
            pltpu.VMEM((4 * BATCHES, RANKS, SLOTS, width), BF16),
            pltpu.VMEM((RANKS * SLOTS, ff), BF16),
            pltpu.VMEM((4 * BATCHES, RANKS, SLOTS, width), BF16),
            pltpu.VMEM((BATCHES, 4, RANKS, SLOTS, width), BF16),
            pltpu.VMEM((BATCHES * RANKS * GROUP_SLOTS, rows), BF16),
            pltpu.VMEM((BATCHES * RANKS, GROUP_SLOTS, 128), BF16),
            pltpu.VMEM((BATCHES * RANKS, GROUP_SLOTS, 128), BF16),
            pltpu.VMEM((BATCHES, RANKS, GROUP_SLOTS, width), BF16),
            pltpu.VMEM((BATCHES, RANKS, GROUP_SLOTS, width), BF16),
            dma((3,)), dma((4,)), pltpu.SemaphoreType.REGULAR, dma((4,)), dma((4,)), dma, dma, dma, dma,
            dma((2,)), dma((4 * BATCHES,)),
            dma, dma((BATCHES,)), dma((2,)), dma((BATCHES, 2)), dma((BATCHES,)), dma((BATCHES,)),
        ],
        compiler_params=pltpu.CompilerParams(
            collective_id=0, has_side_effects=True, vmem_limit_bytes=60 << 20
        ),
        name="layer",
    )(tokens, norm_gain.reshape(1, width), expert_ids.T, gates.T, w_gate, w_up, w_down)


def solution(mesh):
    return jax.shard_map(
        shards,
        mesh=mesh,
        in_specs=(
            P("ep", None),
            P(),
            P("ep", None),
            P("ep", None),
            P("ep", None, None),
            P("ep", None, None),
            P("ep", None, None),
        ),
        out_specs=P("ep", None),
        check_vma=False,
    )
```

```python
import jax
import jax.numpy as jnp
from jax import lax
from jax.experimental import pallas as pl
from jax.experimental.pallas import tpu as pltpu
from jax.sharding import PartitionSpec as P

EPS = 1e-06
F32 = jnp.float32
BF16 = jnp.bfloat16
MESH = pl.DeviceIdType.MESH
SLOTS = 8
GROUP_SLOTS = 16
BATCHES = 4
RANKS = 8


def iota(shape, dim):
    return lax.broadcasted_iota(jnp.int32, shape, dim)


def ones_where(mask):
    return jnp.where(mask, 1.0, 0.0).astype(BF16)


def dot(a, b):
    return jnp.dot(a, b, preferred_element_type=F32)


def turns(batch):
    return batch ^ (batch >> 1)


def peer(me, batch, core, rank):
    dy = rank & 3
    x = ((me >> 1) & 3) ^ (3 * (rank >> 2))
    y = (((me >> 3) & 3) + dy) & 3
    z = ((me >> 5) + turns(batch) - dy) & 3
    return (z << 5) | (y << 3) | (x << 1) | ((me & 1) ^ core)


def expert_slots(ids_ref):
    rows = ids_ref.shape[1]
    first, second = ids_ref[0:1, :], ids_ref[1:2, :]
    expert = iota((128, rows), 0)
    is_first, is_second = expert == first, expert == second
    before = ones_where(iota((rows, rows), 0) < iota((rows, rows), 1))
    rank = dot(ones_where(is_first | is_second), before)
    slot_first = jnp.sum(jnp.where(is_first, rank, 0.0), axis=0, keepdims=True).astype(jnp.int32)
    slot_second = jnp.sum(jnp.where(is_second, rank, 0.0), axis=0, keepdims=True).astype(jnp.int32)
    return first, second, slot_first, slot_second


def normalize(tokens_ref, gain_ref, normed_ref, start, count):
    rows = pl.ds(start, count)
    floats = tokens_ref[rows, :].astype(F32)
    mean = jnp.sum(floats * floats, axis=1, keepdims=True) * (1.0 / floats.shape[1])
    normed_ref[rows, :] = (floats * lax.rsqrt(mean + EPS) * gain_ref[...]).astype(BF16)


def choose(me, ids_ref, chosen_ref):
    count, rows = chosen_ref.shape
    first, second, slot_first, slot_second = expert_slots(ids_ref)
    row = iota((count, rows), 0)
    wanted = peer(me, row >> 7, (row >> 6) & 1, (row >> 3) & 7) * SLOTS + (row & 7)
    chosen_ref[...] = ones_where((wanted == first * SLOTS + slot_first) | (wanted == second * SLOTS + slot_second))


def lay_out(chosen_ref, normed_ref, out_ref, half):
    blocks = out_ref.shape[0] // 2
    rows = pl.ds(half * blocks * SLOTS, blocks * SLOTS)
    for start in range(0, normed_ref.shape[1], 512):
        columns = pl.ds(start, 512)
        block = dot(chosen_ref[rows, :], normed_ref[:, columns]).astype(BF16)
        out_ref[pl.ds(half * blocks, blocks), :, columns] = block.reshape(blocks, SLOTS, 512)


def describe(me, ids_ref, gates_ref, places_ref, meta_ref):
    rows = ids_ref.shape[1]
    first, second, slot_first, slot_second = expert_slots(ids_ref)
    group = first >> 2
    in_group = iota((32, rows), 0) == group
    before = ones_where(iota((rows, rows), 0) < iota((rows, rows), 1))
    rank = dot(ones_where(in_group), before)
    place = jnp.sum(jnp.where(in_group, rank, 0.0), axis=0, keepdims=True).astype(jnp.int32)
    side = ((me >> 1) ^ (me >> 2)) & 1
    relay = (((group & 1) ^ side) << 1) | (me & 1)
    source_first = ((first ^ relay) & 3) * 64 + slot_first
    source_second = ((second ^ relay) & 3) * 64 + slot_second
    count = BATCHES * RANKS * GROUP_SLOTS
    row = iota((count, rows), 0)
    wanted = (peer(me, row >> 7, 0, (row >> 4) & 7) >> 2) * GROUP_SLOTS + (row & 15)
    places = ones_where(wanted == group * GROUP_SLOTS + place)
    places_ref[...] = places
    values = [source_first.astype(F32), source_second.astype(F32)]
    for k in range(2):
        rest = gates_ref[k : k + 1, :]
        for _ in range(3):
            part = rest.astype(BF16).astype(F32)
            values.append(part)
            rest = rest - part
    kind = iota((128, rows), 0)
    table = jnp.zeros((128, rows), F32)
    for k, value in enumerate(values):
        table = jnp.where(kind == k, value, table)
    meta = lax.dot_general(places, table.astype(BF16), (((1,), (1,)), ((), ())), preferred_element_type=F32)
    meta_ref[...] = meta.astype(BF16).reshape(BATCHES * RANKS, GROUP_SLOTS, 128)


def layer_kernel(
    tokens_ref, gain_hbm, ids_hbm, gates_hbm, w_gate_ref, w_up_ref, w_down_ref, out_ref,
    gate_w, up_w, down_w, gain_ref, ids_ref, gates_ref, own_tokens, near_tokens, near_ids, normed, chosen, packed,
    arrived, hidden, produced, gathered, places, meta_out, meta_in, sums, returned, total,
    weight_sem, load_sem, turn_sem, raw_send, raw_recv, ids_send, ids_recv, meta_send, meta_recv,
    packed_send, arrived_recv, core_send, core_recv, cross_send, cross_recv, sums_send, returned_recv,
):
    me = lax.axis_index("ep")
    core = me & 1
    rows, width = own_tokens.shape
    ff = hidden.shape[1]
    per_wave = BATCHES * 2 * RANKS

    barrier = pltpu.get_barrier_semaphore()

    def greet(device):
        pl.semaphore_signal(barrier, inc=1, device_id=(device,), device_id_type=MESH)

    def greet_plane(i, carry):
        plane = ((me + (i << 5)) & 96) | ((me + ((i >> 2) << 3)) & 24)
        for flip in (7, 6, 1):
            greet(plane | ((me & 7) ^ flip))

        @pl.when(i != 0)
        def _():
            greet(plane | (me & 7))

        return carry

    lax.fori_loop(0, 16, greet_plane, 0)
    greet(me ^ 2)
    greet(me ^ 3)

    loads = [
        pltpu.make_async_copy(ids_hbm, ids_ref, load_sem.at[0]),
        pltpu.make_async_copy(tokens_ref, own_tokens, load_sem.at[1]),
        pltpu.make_async_copy(gain_hbm, gain_ref, load_sem.at[2]),
        pltpu.make_async_copy(gates_hbm, gates_ref, load_sem.at[3]),
    ]
    weights = [
        pltpu.make_async_copy(w_gate_ref.at[0], gate_w, weight_sem.at[0]),
        pltpu.make_async_copy(w_up_ref.at[0], up_w, weight_sem.at[1]),
        pltpu.make_async_copy(w_down_ref.at[0], down_w, weight_sem.at[2]),
    ]
    for copy in loads:
        copy.start()

    chunks = [(0, 3 * rows // 8), (3 * rows // 8, 3 * rows // 8), (3 * rows // 4, rows // 8), (7 * rows // 8, rows // 8)]
    raw = [
        pltpu.make_async_remote_copy(
            tokens_ref.at[pl.ds(start, count)], near_tokens.at[pl.ds(start, count)], raw_send.at[k], raw_recv.at[k],
            device_id=(me ^ 2,), device_id_type=MESH,
        )
        for k, (start, count) in enumerate(chunks)
    ]
    raw_ids = pltpu.make_async_remote_copy(
        ids_hbm, near_ids, ids_send, ids_recv, device_id=(me ^ 2,), device_id_type=MESH
    )

    def send_packed(wave, half):
        first_unit = BATCHES * (3 * core if wave == 0 else 1 + core)
        blocks = per_wave // 2

        def send(i, carry):
            batch, rank = i >> 4, i & 7
            pltpu.make_async_remote_copy(
                packed.at[wave, i], arrived.at[first_unit + batch, rank],
                packed_send.at[wave], arrived_recv.at[first_unit + batch],
                device_id=(peer(me, batch, (i >> 3) & 1, rank),), device_id_type=MESH,
            ).start()
            return carry

        lax.fori_loop(max(1, half * blocks), (half + 1) * blocks, send, 0)
        if half == 0:
            arrived[first_unit, 0] = packed[wave, 0]

    def wait_barrier():
        with jax.named_scope("barrier"):
            pl.semaphore_wait(barrier, per_wave + 1)

    wait_barrier()
    raw_ids.start()

    @pl.when(core == 0)
    def _():
        for copy in raw:
            copy.start()

    for copy in loads:
        copy.wait()
    for copy in weights:
        copy.start()
    with jax.named_scope("pack_own"):
        choose(me, ids_ref, chosen)
        normalize(own_tokens, gain_ref, normed, 0, rows)
        for half in range(2):
            lay_out(chosen, normed, packed.at[0], half)

            @pl.when(core == 0)
            def _():
                send_packed(0, half)

    with jax.named_scope("describe"):
        describe(me, ids_ref, gates_ref, places, meta_out)

    def send_meta(i, carry):
        pltpu.make_async_remote_copy(
            meta_out.at[i], meta_in.at[i], meta_send, meta_recv,
            device_id=(peer(me, i >> 3, 0, i & 7),), device_id_type=MESH,
        ).start()
        return carry

    lax.fori_loop(1, BATCHES * RANKS, send_meta, 0)
    meta_in[0] = meta_out[0]
    with jax.named_scope("ids_wait"):
        raw_ids.wait_recv()
        choose(me, near_ids, chosen)

    @pl.when(core == 1)
    def _():
        with jax.named_scope("turn"):
            pl.semaphore_wait(turn_sem, 1)
        for copy in raw:
            copy.start()

    def near():
        for k, (start, count) in enumerate(chunks):
            with jax.named_scope("raw_wait"):
                raw[k].wait_recv()

            if k == 2:
                @pl.when(core == 0)
                def _():
                    pl.semaphore_signal(turn_sem, inc=1, device_id=(me ^ 1,), device_id_type=MESH)

            normalize(near_tokens, gain_ref, normed, start, count)
        with jax.named_scope("pack_near"):
            lay_out(chosen, normed, packed.at[1], 0)
            send_packed(1, 0)
            lay_out(chosen, normed, packed.at[1], 1)
            send_packed(1, 1)

        @pl.when(core == 1)
        def _():
            send_packed(0, 0)
            send_packed(0, 1)

    def wait_unit(unit, batch, source_core):
        alone = (batch == 0) & (source_core == core)

        @pl.when(alone)
        def _():
            view = arrived.at[unit, pl.ds(1, RANKS - 1)]
            pltpu.make_async_copy(view, view, arrived_recv.at[unit]).wait()

        @pl.when(jnp.logical_not(alone))
        def _():
            view = arrived.at[unit]
            pltpu.make_async_copy(view, view, arrived_recv.at[unit]).wait()

    def expert(unit, carry):
        @pl.when(unit == 6 * core)
        def _():
            near()

        batch, kind = unit & 3, unit >> 2
        source_core = kind >> 1
        crossing = (kind == 1) | (kind == 2)
        with jax.named_scope("unit_wait"):
            wait_unit(unit, batch, source_core)

        @pl.when(unit == 0)
        def _():
            for copy in weights:
                copy.wait()

        with jax.named_scope("unit"):
            block_rows = arrived[unit].reshape(RANKS * SLOTS, width)
            for start in range(0, ff, 256):
                columns = pl.ds(start, 256)
                gate_part = dot(block_rows, gate_w[:, columns])
                up_part = dot(block_rows, up_w[:, columns])
                hidden[:, columns] = (gate_part / (1.0 + jnp.exp(-gate_part)) * up_part).astype(BF16)
            for start in range(0, width, 256):
                columns = pl.ds(start, 256)
                block = dot(hidden[...], down_w[:, columns]).astype(BF16)
                produced[unit, :, :, columns] = block.reshape(RANKS, SLOTS, 256)

        other = source_core ^ core

        @pl.when(crossing)
        def _():
            pltpu.make_async_remote_copy(
                produced.at[unit], gathered.at[batch, 2 + other],
                cross_send.at[source_core], cross_recv.at[batch, other],
                device_id=(me ^ (2 + other),), device_id_type=MESH,
            ).start()

        @pl.when(jnp.logical_not(crossing) & (other == 1))
        def _():
            pltpu.make_async_remote_copy(
                produced.at[unit], gathered.at[batch, 1], core_send, core_recv.at[batch],
                device_id=(me ^ 1,), device_id_type=MESH,
            ).start()

        @pl.when(jnp.logical_not(crossing) & (other == 0))
        def _():
            gathered[batch, 0] = produced[unit]

        @pl.when(((core == 0) & (unit >= 8) & (unit < 12)) | (core == 1) & (unit >= 12))
        def _():
            relay(batch)

        return carry

    def relay(batch):
        with jax.named_scope("relay_wait"):
            @pl.when(batch == 0)
            def _():
                view = meta_in.at[pl.ds(1, BATCHES * RANKS - 1)]
                pltpu.make_async_copy(view, view, meta_recv).wait()

            view = gathered.at[batch, 1]
            pltpu.make_async_copy(view, view, core_recv.at[batch]).wait()
            for other in range(2):
                view = gathered.at[batch, 2 + other]
                pltpu.make_async_copy(view, view, cross_recv.at[batch, other]).wait()
        count = RANKS * GROUP_SLOTS
        meta = meta_in[pl.ds(batch * RANKS, RANKS)].reshape(count, 128).astype(F32)
        base = (iota((count, 1), 0) // GROUP_SLOTS) * SLOTS
        column = iota((count, 4 * RANKS * SLOTS), 1)
        picks = [ones_where(column == meta[:, k : k + 1].astype(jnp.int32) + base) for k in range(2)]
        scale = [meta[:, k : k + 1] + meta[:, k + 1 : k + 2] + meta[:, k + 2 : k + 3] for k in (2, 5)]
        for start in range(0, width, 512):
            columns = pl.ds(start, 512)
            rows = gathered[batch, :, :, :, columns].reshape(4 * RANKS * SLOTS, 512)
            total = dot(picks[0], rows) * scale[0] + dot(picks[1], rows) * scale[1]
            sums[batch, :, :, columns] = total.astype(BF16).reshape(RANKS, GROUP_SLOTS, 512)

        def send(rank, carry):
            pltpu.make_async_remote_copy(
                sums.at[batch, rank], returned.at[batch, rank], sums_send.at[batch], returned_recv.at[batch],
                device_id=(back(batch, rank),), device_id_type=MESH,
            ).start()
            return carry

        @pl.when(batch == 0)
        def _():
            returned[0, 0] = sums[0, 0]
            lax.fori_loop(1, RANKS, send, 0)

        @pl.when(batch != 0)
        def _():
            lax.fori_loop(0, RANKS, send, 0)

    def back(batch, rank):
        dy = rank & 3
        x = ((me >> 1) & 3) ^ (3 * (rank >> 2))
        y = (((me >> 3) & 3) - dy) & 3
        z = ((me >> 5) - turns(batch) + dy) & 3
        return (z << 5) | (y << 3) | (x << 1) | (me & 1)

    lax.fori_loop(0, 4 * BATCHES, expert, 0)

    def wait_returned(batch):
        view = returned.at[batch, pl.ds(1, RANKS - 1)] if batch == 0 else returned.at[batch]
        pltpu.make_async_copy(view, view, returned_recv.at[batch]).wait()

    def bring(start, stop, columns):
        count = RANKS * GROUP_SLOTS
        back_rows = returned[start:stop, :, :, columns].reshape((stop - start) * count, 512)
        return lax.dot_general(
            places[start * count : stop * count], back_rows, (((0,), (0,)), ((), ())), preferred_element_type=F32
        )

    last = BATCHES - 1
    for batch in range(last):
        wait_returned(batch)
    for start in range(0, width, 512):
        columns = pl.ds(start, 512)
        total[:, columns] = bring(0, last, columns)
    with jax.named_scope("return_wait"):
        wait_returned(last)
    for start in range(0, width, 512):
        columns = pl.ds(start, 512)
        out_ref[:, columns] = (total[:, columns] + bring(last, BATCHES, columns)).astype(BF16)

    for copy in raw:
        copy.wait_send()
    raw_ids.wait_send()

    def drain(view, sem):
        pltpu.make_async_copy(view, view, sem).wait()

    for wave in range(2):
        drain(packed.at[wave, pl.ds(1, per_wave - 1)], packed_send.at[wave])
    drain(meta_out.at[pl.ds(1, BATCHES * RANKS - 1)], meta_send)
    drain(gathered.at[:, 1], core_send)
    for source_core in range(2):
        drain(gathered.at[:, 2], cross_send.at[source_core])
    for batch in range(BATCHES):
        drain(sums.at[batch, pl.ds(1, RANKS - 1)] if batch == 0 else sums.at[batch], sums_send.at[batch])


def whole():
    return pl.BlockSpec(memory_space=pltpu.VMEM)


def shards(tokens, norm_gain, expert_ids, gates, w_gate, w_up, w_down):
    rows, width = tokens.shape
    ff = w_gate.shape[2]
    dma = pltpu.SemaphoreType.DMA
    return pl.pallas_call(
        layer_kernel,
        out_shape=jax.ShapeDtypeStruct((rows, width), BF16),
        in_specs=[pl.BlockSpec(memory_space=pltpu.HBM)] * 7,
        out_specs=whole(),
        scratch_shapes=[
            pltpu.VMEM((width, ff), BF16),
            pltpu.VMEM((width, ff), BF16),
            pltpu.VMEM((ff, width), BF16),
            pltpu.VMEM((1, width), F32),
            pltpu.VMEM((2, rows), jnp.int32),
            pltpu.VMEM((2, rows), F32),
            pltpu.VMEM((rows, width), BF16),
            pltpu.VMEM((rows, width), BF16),
            pltpu.VMEM((2, rows), jnp.int32),
            pltpu.VMEM((rows, width), BF16),
            pltpu.VMEM((BATCHES * 2 * RANKS * SLOTS, rows), BF16),
            pltpu.VMEM((2, BATCHES * 2 * RANKS, SLOTS, width), BF16),
            pltpu.VMEM((4 * BATCHES, RANKS, SLOTS, width), BF16),
            pltpu.VMEM((RANKS * SLOTS, ff), BF16),
            pltpu.VMEM((4 * BATCHES, RANKS, SLOTS, width), BF16),
            pltpu.VMEM((BATCHES, 4, RANKS, SLOTS, width), BF16),
            pltpu.VMEM((BATCHES * RANKS * GROUP_SLOTS, rows), BF16),
            pltpu.VMEM((BATCHES * RANKS, GROUP_SLOTS, 128), BF16),
            pltpu.VMEM((BATCHES * RANKS, GROUP_SLOTS, 128), BF16),
            pltpu.VMEM((BATCHES, RANKS, GROUP_SLOTS, width), BF16),
            pltpu.VMEM((BATCHES, RANKS, GROUP_SLOTS, width), BF16),
            pltpu.VMEM((rows, width), F32),
            dma((3,)), dma((4,)), pltpu.SemaphoreType.REGULAR, dma((4,)), dma((4,)), dma, dma, dma, dma,
            dma((2,)), dma((4 * BATCHES,)),
            dma, dma((BATCHES,)), dma((2,)), dma((BATCHES, 2)), dma((BATCHES,)), dma((BATCHES,)),
        ],
        compiler_params=pltpu.CompilerParams(
            collective_id=0, has_side_effects=True, vmem_limit_bytes=60 << 20
        ),
        name="layer",
    )(tokens, norm_gain.reshape(1, width), expert_ids.T, gates.T, w_gate, w_up, w_down)


def solution(mesh):
    return jax.shard_map(
        shards,
        mesh=mesh,
        in_specs=(
            P("ep", None),
            P(),
            P("ep", None),
            P("ep", None),
            P("ep", None, None),
            P("ep", None, None),
            P("ep", None, None),
        ),
        out_specs=P("ep", None),
        check_vma=False,
    )
```
